512 devices in a mesh: grp: 2 (over y), kv: 16 (over z), tp: 16 (over x, core).
Axes of the slice: x: 8, y: 2, z: 16, core: 2. Of those that a mesh axis runs over, the one named last changes fastest.
The devices are a block of a 8x16x16 slice.
Arguments:
- tokens: bfloat16 [640, 4096], P('grp', ('kv', 'tp')), parts along dimension 0, may hold values from -65 to 65
- lengths: int32 [640], P(('grp', 'kv')), parts along dimension 0, may hold values from 1 to 16384, 1310720 in all
- memory: float32 [640, 16, 128, 128], P(('grp', 'kv'), 'tp'), parts along dimension 0, may hold values from -6 to 6
- norm_attn: bfloat16 [4096], P('kv'), may hold values from 0.099609375 to 1.8984375
- w_query: bfloat16 [4096, 2048], P('kv', 'tp'), may hold values from -0.09375 to 0.09375
- w_key: bfloat16 [4096, 2048], P('kv', 'tp'), may hold values from -0.09375 to 0.09375
- w_value: bfloat16 [4096, 2048], P('kv', 'tp'), may hold values from -0.09375 to 0.09375
- w_gate: bfloat16 [4096, 2048], P('kv', 'tp'), may hold values from -0.09375 to 0.09375
- head_gain: bfloat16 [2048], P('tp'), may hold values from 0.099609375 to 1.8984375
- w_out: bfloat16 [2048, 4096], P('tp', 'kv'), may hold values from -0.1875 to 0.1875
- norm_mlp: bfloat16 [4096], P('kv'), may hold values from 0.099609375 to 1.8984375
- w_gate_mlp: bfloat16 [4096, 14336], P('kv', 'tp'), may hold values from -0.09375 to 0.09375
- w_up: bfloat16 [4096, 14336], P('kv', 'tp'), may hold values from -0.09375 to 0.09375
- w_down: bfloat16 [14336, 4096], P('tp', 'kv'), may hold values from -0.0625 to 0.0625
Outputs:
- result: bfloat16 [640, 4096], P('grp', ('kv', 'tp')), parts along dimension 0
- new_memory: float32 [640, 16, 128, 128], P(('grp', 'kv'), 'tp'), parts along dimension 0
The draws below stay inside these ranges and needn't reach their ends.
There are 2 independent parts, one for each index of `grp`. The reference program is written for one: setup_inputs(seed, part) draws one part's arguments, and reference() takes and returns one part's arrays. A program takes and returns all parts, laid end to end along the dimension named above; an argument that names none is the same for every part. Nothing has to cross between parts.
Inputs may be any that keep to these rules, and one draw needn't show every extreme that they name: Within each part along grp the lengths sum to 1310720 and the longest is exactly 16384.
All inputs are finite; a program needn't handle non-finite values. No bound on the sum of `lengths` on one device may be relied on, other than what follows from the above.
Results may differ from the reference program's by a relative error of at most 0.025.
Values may be sent and summed in bfloat16 or wider, within the bound.
No kernel may reach another device: no remote copies, remote signals or barrier semaphores. Data moves between devices by JAX's collectives and lax.ppermute only.
A program may use at most 64 MiB of HBM per device.

```python
import math
import jax
import jax.numpy as jnp
import numpy as np
from jax import lax

D = 4096
HEADS = 16
HEAD = 128
FF = 14336
MAXLEN = 16384
BATCH = 320
RET_WIDTH = 2048


def draw_tokens(key, part):
    noise = jnp.clip(jax.random.normal(jax.random.fold_in(key, 1), (BATCH, D), jnp.float32), -6.0, 6.0)
    column = jnp.arange(D, dtype=jnp.float32) / D
    values = noise * (3.0 ** column)[None, :] * 0.6
    return values.astype(jnp.bfloat16)


def raised(array, stream_key, source, target, blocks, factor):
    def block_of(axis_at):
        return (jnp.arange(array.shape[axis_at]) // (array.shape[axis_at] // blocks)).reshape((-1,) + (1,) * (array.ndim - 1 - axis_at))

    one_side = jax.random.permutation(stream_key, blocks)[block_of(target)]
    far = (block_of(target) + blocks // 2) % blocks
    return jnp.where((block_of(source) == one_side) | (block_of(source) == far), factor * array, array)


def steps_of(own_key, shape, split, least, top_value):
    def one(axis_at, parts):
        draws = jax.random.uniform(jax.random.fold_in(jax.random.fold_in(own_key, 6), axis_at), (parts,), jnp.float32, least / len(split), top_value / len(split))
        return jnp.repeat(jnp.exp(draws), shape[axis_at] // parts).reshape((-1,) + (1,) * (len(shape) - axis_at - 1))

    gain = one(*split[0])
    for cut in split[1:]:
        gain = gain * one(*cut)
    return gain


def length_profile(number_of, total, most, lean):
    loads = [(1 << 20) // math.isqrt(rank ** lean) + 1 for rank in range(2, number_of + 1)]
    surplus, holding = total - most - (number_of - 1), [1] * (number_of - 1)
    while surplus > 0:
        candidates = [i for i in range(number_of - 1) if holding[i] < most]
        mass, budget = sum([loads[i] for i in candidates]), surplus
        for i in candidates:
            addition = min(most - holding[i], max(1, budget * loads[i] // mass), surplus)
            holding[i] = holding[i] + addition
            surplus = surplus - addition
    return np.array([most] + holding)


def ragged_sizes(stream_key, count, total, limit, slope):
    if count == 2:
        one = jax.random.randint(stream_key, (), max(1, total - limit), min(limit, total - 1) + 1)
        return jnp.stack([one, total - one])
    tallies = jnp.asarray(length_profile(count, total, limit, slope), jnp.int32)
    pairs = (count - 1) // 2
    donor, sink = tallies[1:1 + 2 * pairs:2], tallies[2:2 + 2 * pairs:2]
    slack = jnp.minimum(donor - 1, limit - sink)
    moved = jax.random.randint(jax.random.fold_in(stream_key, 1), (pairs,), 0, 1 << 20) % (slack + 1)
    tallies = tallies.at[1:1 + 2 * pairs:2].set(donor - moved).at[2:2 + 2 * pairs:2].set(sink + moved)
    return tallies[jax.random.permutation(jax.random.fold_in(stream_key, 2), count)]


def normal_values(own_key, extent, width, most, pieces=(), held_as=jnp.bfloat16):
    array = width * jax.random.normal(own_key, extent, jnp.float32)
    if pieces:
        array = array * steps_of(own_key, extent, pieces, -0.22, 0.18)
    return jnp.clip(array, -most, most).astype(held_as)


def noise_with(own_key, dims, deviation, limit, pieces, heavy, kind=jnp.bfloat16):
    values = deviation * jax.random.normal(own_key, dims, jnp.float32)
    if pieces:
        values = values * steps_of(own_key, dims, pieces, -0.22, 0.18)
    return jnp.clip(raised(values, jax.random.fold_in(own_key, 3), *heavy), -limit, limit).astype(kind)


def setup_inputs(seed: int = 0, part: int = 0) -> dict:
    arg_keys = jax.random.split(jax.random.key(seed), 15)
    own_keys = jax.random.split(jax.random.fold_in(arg_keys[14], part), 15)
    tokens = draw_tokens(jax.random.fold_in(jax.random.fold_in(arg_keys[14], part), 71), part)
    lengths = ragged_sizes(own_keys[1], BATCH, BATCH * MAXLEN // 4, MAXLEN, 2).astype(jnp.int32)
    memory = normal_values(own_keys[2], (BATCH, HEADS, HEAD, HEAD), 1.0, 6.0, ((0, 16), (1, 16)), jnp.float32)
    norm_attn = jnp.clip(1.0 + 0.18 * jax.random.normal(arg_keys[3], (D,), jnp.float32), 0.099609375, 1.8984375).astype(jnp.bfloat16)
    w_query = normal_values(arg_keys[4], (D, RET_WIDTH), D ** -0.5, 0.09375, ((0, 16), (1, 16)))
    w_key = normal_values(arg_keys[5], (D, RET_WIDTH), D ** -0.5, 0.09375, ((0, 16), (1, 16)))
    w_value = normal_values(arg_keys[6], (D, RET_WIDTH), D ** -0.5, 0.09375, ((0, 16), (1, 16)))
    w_gate = normal_values(arg_keys[7], (D, RET_WIDTH), D ** -0.5, 0.09375, ((0, 16), (1, 16)))
    head_gain = jnp.clip(1.0 + 0.18 * jax.random.normal(arg_keys[8], (RET_WIDTH,), jnp.float32), 0.099609375, 1.8984375).astype(jnp.bfloat16)
    w_out = noise_with(arg_keys[9], (RET_WIDTH, D), RET_WIDTH ** -0.5, 0.1875, ((0, 16), (1, 16)), (0, 1, 16, 2.0))
    norm_mlp = jnp.clip(1.0 + 0.18 * jax.random.normal(arg_keys[10], (D,), jnp.float32), 0.099609375, 1.8984375).astype(jnp.bfloat16)
    w_gate_mlp = normal_values(arg_keys[11], (D, FF), D ** -0.5, 0.09375, ((0, 16), (1, 16)))
    w_up = normal_values(arg_keys[12], (D, FF), D ** -0.5, 0.09375, ((0, 16), (1, 16)))
    w_down = noise_with(arg_keys[13], (FF, D), FF ** -0.5, 0.0625, ((0, 16), (1, 16)), (0, 1, 16, 2.0))
    return dict(tokens=tokens, lengths=lengths, memory=memory, norm_attn=norm_attn, w_query=w_query, w_key=w_key, w_value=w_value, w_gate=w_gate, head_gain=head_gain, w_out=w_out, norm_mlp=norm_mlp, w_gate_mlp=w_gate_mlp, w_up=w_up, w_down=w_down)


epsilon = 1e-06

def rotate(values, position):
    half_width = values.shape[-1] // 2
    inverse = 10000.0 ** (-jnp.arange(half_width, dtype=jnp.float32) / half_width)
    angles = position[:, None] * inverse[None, :]
    cosine = jnp.cos(angles)[:, None, :]
    sine = jnp.sin(angles)[:, None, :]
    first = values[..., :half_width]
    second = values[..., half_width:]
    return jnp.concatenate([first * cosine - second * sine, second * cosine + first * sine], axis=-1)

def head_decay(head_index):
    exponent = -5.0 - head_index.astype(jnp.float32) * (7.0 / max(HEADS - 1, 1))
    return 1.0 - jnp.exp2(exponent)

def retain(memory, queries, key_rows, value_rows, gate_rows, head_gain, decay_rate):
    new_memory = decay_rate[None, :, None, None] * memory + key_rows[:, :, :, None] * value_rows[:, :, None, :]
    readout = jnp.einsum('bhd,bhde->bhe', queries * queries.shape[-1] ** (-0.5), new_memory, precision=lax.Precision.HIGHEST)
    centred = readout - lax.optimization_barrier(jnp.mean(readout, axis=-1, keepdims=True))
    normed = centred * lax.rsqrt(lax.optimization_barrier(jnp.mean(centred * centred, axis=-1, keepdims=True)) + epsilon)
    normed = normed.reshape(readout.shape[0], -1) * head_gain.astype(jnp.float32)
    return (new_memory, (normed * jax.nn.silu(gate_rows)).astype(jnp.bfloat16))

def reference(tokens, lengths, memory, norm_attn, w_query, w_key, w_value, w_gate, head_gain, w_out, norm_mlp, w_gate_mlp, w_up, w_down):
    tok_float = tokens.astype(jnp.float32)
    inv_attn = lax.rsqrt(lax.optimization_barrier(jnp.sum(tok_float * tok_float, axis=1)) / D + epsilon)
    scaled = (tok_float * norm_attn.astype(jnp.float32)).astype(jnp.bfloat16)

    def project(weight):
        return inv_attn[:, None] * jnp.dot(scaled, weight, preferred_element_type=jnp.float32)
    position = lengths.astype(jnp.float32)
    batch_rows = tokens.shape[0]
    queries = rotate(project(w_query).reshape(batch_rows, HEADS, HEAD), position)
    key_rows = rotate(project(w_key).reshape(batch_rows, HEADS, HEAD), position)
    value_rows = project(w_value).reshape(batch_rows, HEADS, HEAD)
    gate_rows = project(w_gate)
    decay_rate = head_decay(jnp.arange(HEADS))
    new_memory, mixed = retain(memory, queries, key_rows, value_rows, gate_rows, head_gain, decay_rate)
    middle = (tok_float + jnp.dot(mixed, w_out, preferred_element_type=jnp.float32)).astype(jnp.bfloat16)
    mid_float = middle.astype(jnp.float32)
    inv_mlp = lax.rsqrt(lax.optimization_barrier(jnp.sum(mid_float * mid_float, axis=1)) / D + epsilon)
    scaled_mid = (mid_float * norm_mlp.astype(jnp.float32)).astype(jnp.bfloat16)
    gate_mlp = inv_mlp[:, None] * jnp.dot(scaled_mid, w_gate_mlp, preferred_element_type=jnp.float32)
    up_rows = inv_mlp[:, None] * jnp.dot(scaled_mid, w_up, preferred_element_type=jnp.float32)
    hidden = (jax.nn.silu(gate_mlp) * up_rows).astype(jnp.bfloat16)
    result = (mid_float + jnp.dot(hidden, w_down, preferred_element_type=jnp.float32)).astype(jnp.bfloat16)
    return (result, new_memory)
```

```python
import jax
import jax.numpy as jnp
from jax import lax
from jax.sharding import PartitionSpec as P


D = 4096
HEADS = 16


epsilon = 1e-06


def from_everyone(array, axis):
    copies = jnp.broadcast_to(array, (lax.axis_size(axis), *array.shape))
    return lax.all_to_all(copies, axis, split_axis=0, concat_axis=0, tiled=True)


def in_three(values):
    high = values.astype(jnp.bfloat16)
    rest = values - high.astype(jnp.float32)
    mid = rest.astype(jnp.bfloat16)
    low = (rest - mid.astype(jnp.float32)).astype(jnp.bfloat16)
    return high, mid, low


def rotate(values, cosine, sine):
    half_width = values.shape[-1] // 2
    first = values[..., :half_width]
    second = values[..., half_width:]
    return jnp.concatenate(
        [first * cosine - second * sine, second * cosine + first * sine], axis=-1
    )


def head_decay(head_index):
    exponent = -5.0 - head_index.astype(jnp.float32) * (7.0 / max(HEADS - 1, 1))
    return 1.0 - jnp.exp2(exponent)


def retain(memory, queries, key_rows, value_rows, gate_rows, head_gain, decay_rate):
    new_memory = (
        decay_rate[None, :, None, None] * memory
        + key_rows[:, :, :, None] * value_rows[:, :, None, :]
    )
    readout = jnp.einsum(
        "bhd,bhde->bhe",
        queries * queries.shape[-1] ** (-0.5),
        new_memory,
        precision=lax.Precision.HIGHEST,
    )
    centred = readout - jnp.mean(readout, axis=-1, keepdims=True)
    normed = centred * lax.rsqrt(jnp.mean(centred * centred, axis=-1, keepdims=True) + epsilon)
    normed = normed.reshape(readout.shape[0], -1) * head_gain.astype(jnp.float32)
    return (new_memory, (normed * jax.nn.silu(gate_rows)).astype(jnp.bfloat16))


def per_device(
    tokens,
    lengths,
    memory,
    norm_attn,
    w_query,
    w_key,
    w_value,
    w_gate,
    head_gain,
    w_out,
    norm_mlp,
    w_gate_mlp,
    w_up,
    w_down,
):
    f32, bf16 = jnp.float32, jnp.bfloat16
    n_kv, n_tp = lax.axis_size("kv"), lax.axis_size("tp")
    kv = lax.axis_index("kv")
    rows = tokens.shape[0]
    own = memory.shape[0]
    heads_local = memory.shape[1]
    head_size = memory.shape[2]
    width = w_query.shape[1]
    block = w_query.shape[0]
    ff = w_up.shape[1]

    tok = tokens.T
    gathered = from_everyone(tok, "tp").reshape(block, rows).astype(f32)
    squares = jnp.sum(gathered * gathered, axis=0)
    scaled = (gathered * norm_attn.astype(f32)[:, None]).astype(bf16)
    parts = jnp.concatenate(
        [
            lax.dot_general(scaled, w, (((0,), (0,)), ((), ())), preferred_element_type=f32)
            for w in (w_query, w_key, w_value, w_gate)
        ],
        axis=1,
    ).astype(bf16)
    terms = jnp.stack([t.reshape(n_kv, own) for t in in_three(squares)], axis=1)
    terms = jnp.pad(terms, ((0, 0), (0, 1), (0, parts.shape[1] - own)))
    sent = jnp.concatenate([parts.reshape(n_kv, own, -1), terms], axis=1)
    got = lax.all_to_all(sent, "kv", 0, 0, tiled=True)
    summed = jnp.sum(got.astype(f32), axis=0)
    own_squares = summed[own, :own] + summed[own + 1, :own] + summed[own + 2, :own]
    projected = summed[:own] * lax.rsqrt(own_squares / D + epsilon)[:, None]

    half = head_size // 2
    inverse = 10000.0 ** (-jnp.arange(half, dtype=f32) / half)
    angles = lengths.astype(f32)[:, None] * inverse[None, :]
    cosine, sine = jnp.cos(angles)[:, None, :], jnp.sin(angles)[:, None, :]
    heads = [
        projected[:, i * width : (i + 1) * width].reshape(own, heads_local, head_size)
        for i in range(3)
    ]
    decay_rate = head_decay(lax.axis_index("tp") * heads_local + jnp.arange(heads_local))
    new_memory, mixed = retain(
        memory,
        rotate(heads[0], cosine, sine),
        rotate(heads[1], cosine, sine),
        heads[2],
        projected[:, 3 * width :],
        head_gain,
        decay_rate,
    )

    mixed_all = from_everyone(mixed, "kv").reshape(rows, width)
    attn_part = lax.dot_general(
        w_out, mixed_all, (((0,), (1,)), ((), ())), preferred_element_type=f32
    ).astype(bf16)
    attn = lax.all_to_all(attn_part.reshape(n_tp, -1, rows), "tp", 0, 0, tiled=True)
    middle = (tok.astype(f32) + jnp.sum(attn.astype(f32), axis=0)).astype(bf16)

    mid_all = from_everyone(middle, "tp").reshape(block, rows).astype(f32)
    mid_squares = from_everyone(jnp.sum(mid_all * mid_all, axis=0)[None], "kv")
    scaled_mid = (mid_all * norm_mlp.astype(f32)[:, None]).astype(bf16)
    lanes = 128
    cuts = ff // lanes
    both = jnp.concatenate(
        [w_gate_mlp.reshape(block, cuts, lanes), w_up.reshape(block, cuts, lanes)], axis=2
    ).transpose(1, 0, 2)
    terms = jnp.concatenate(
        [
            lax.dot_general(scaled_mid, both[c], (((0,), (0,)), ((), ())), preferred_element_type=f32)
            for c in range(cuts)
        ],
        axis=0,
    ).astype(bf16)
    terms = lax.psum_scatter(terms, "kv", scatter_dimension=0, tiled=True)
    terms = terms.astype(f32)
    share = terms.shape[0]
    totals = jnp.sum(mid_squares, axis=(0, 1))
    inv_mlp = lax.rsqrt(totals / D + epsilon)
    inv_mlp = lax.dynamic_slice_in_dim(
        jnp.concatenate([inv_mlp, inv_mlp]), lax.rem(kv * share, rows), share, 0
    )[:, None]
    hidden = (jax.nn.silu(inv_mlp * terms[:, :lanes]) * (inv_mlp * terms[:, lanes:])).astype(bf16)
    hidden = lax.all_gather(hidden, "kv", axis=0, tiled=True).reshape(cuts, rows, lanes)
    down = lax.dot_general(
        w_down,
        hidden.transpose(1, 0, 2).reshape(rows, ff),
        (((0,), (1,)), ((), ())),
        preferred_element_type=f32,
    ).astype(bf16)
    down = lax.all_to_all(down.reshape(n_tp, -1, rows), "tp", 0, 0, tiled=True)
    result = (middle.astype(f32) + jnp.sum(down.astype(f32), axis=0)).astype(bf16)
    return (result.T, new_memory)


def solution(mesh):
    in_specs = (
        P("grp", ("kv", "tp")),
        P(("grp", "kv")),
        P(("grp", "kv"), "tp", None, None),
        P("kv"),
        P("kv", "tp"),
        P("kv", "tp"),
        P("kv", "tp"),
        P("kv", "tp"),
        P("tp"),
        P("tp", "kv"),
        P("kv"),
        P("kv", "tp"),
        P("kv", "tp"),
        P("tp", "kv"),
    )
    out_specs = (P("grp", ("kv", "tp")), P(("grp", "kv"), "tp", None, None))
    return jax.shard_map(
        per_device, mesh=mesh, in_specs=in_specs, out_specs=out_specs, check_vma=False
    )
```

```python
import jax
import jax.numpy as jnp
from jax import lax
from jax.experimental import pallas as pl
from jax.experimental.pallas import tpu as pltpu
from jax.sharding import PartitionSpec as P


D = 4096
HEADS = 16


epsilon = 1e-06


def from_everyone(array, axis):
    copies = jnp.broadcast_to(array, (lax.axis_size(axis), *array.shape))
    return lax.all_to_all(copies, axis, split_axis=0, concat_axis=0, tiled=True)


def in_three(values):
    high = values.astype(jnp.bfloat16)
    rest = values - high.astype(jnp.float32)
    mid = rest.astype(jnp.bfloat16)
    low = (rest - mid.astype(jnp.float32)).astype(jnp.bfloat16)
    return high, mid, low


def rotate(values, cosine, sine):
    half_width = values.shape[-1] // 2
    first = values[..., :half_width]
    second = values[..., half_width:]
    return jnp.concatenate(
        [first * cosine - second * sine, second * cosine + first * sine], axis=-1
    )


def head_decay(head_index):
    exponent = -5.0 - head_index.astype(jnp.float32) * (7.0 / max(HEADS - 1, 1))
    return 1.0 - jnp.exp2(exponent)


def retain(memory, queries, key_rows, value_rows, gate_rows, head_gain, decay_rate):
    new_memory = (
        decay_rate[None, :, None, None] * memory
        + key_rows[:, :, :, None] * value_rows[:, :, None, :]
    )
    readout = jnp.einsum(
        "bhd,bhde->bhe",
        queries * queries.shape[-1] ** (-0.5),
        new_memory,
        precision=lax.Precision.HIGHEST,
    )
    centred = readout - jnp.mean(readout, axis=-1, keepdims=True)
    normed = centred * lax.rsqrt(jnp.mean(centred * centred, axis=-1, keepdims=True) + epsilon)
    normed = normed.reshape(readout.shape[0], -1) * head_gain.astype(jnp.float32)
    return (new_memory, (normed * jax.nn.silu(gate_rows)).astype(jnp.bfloat16))


def gate_and_up(order, wide, middle, parts):
    blocks = len(wide)
    units, block = wide[0].shape
    rows = middle.shape[2]
    share = units // (2 * parts)
    tail = 8

    def kernel(order_ref, *refs):
        wide_refs, middle_ref, out_ref = refs[:blocks], refs[blocks], refs[blocks + 1]
        total, squares = None, None
        for m in range(blocks):
            held = middle_ref[order_ref[m]]
            value = held.astype(jnp.float32)
            square = jnp.sum(value * value, axis=0, keepdims=True)
            product = jnp.dot(wide_refs[m][...], held, preferred_element_type=jnp.float32)
            total = product if total is None else total + product
            squares = square if squares is None else squares + square
        total = total.astype(jnp.bfloat16)
        high, mid, low = in_three(squares)
        ones = [high, mid, low, jnp.zeros_like(low)]
        under = jnp.concatenate(
            [
                jnp.concatenate([ones[2 * r].astype(jnp.float32), ones[2 * r + 1].astype(jnp.float32)], axis=1)
                for r in range(2)
            ]
            + [jnp.zeros((tail - 2, 2 * rows), jnp.float32)],
            axis=0,
        ).astype(jnp.bfloat16)
        for a in range(parts):
            for half in range(2):
                start = (half * parts + a) * share
                out_ref[a, :share, half * rows : (half + 1) * rows] = total[start : start + share]
            out_ref[a, share:, :] = under

    vmem = pl.BlockSpec(memory_space=pltpu.VMEM)
    return pl.pallas_call(
        kernel,
        out_shape=jax.ShapeDtypeStruct((parts, share + tail, 2 * rows), jnp.bfloat16),
        in_specs=[pl.BlockSpec(memory_space=pltpu.SMEM)] + [vmem] * (blocks + 1),
        out_specs=vmem,
        name="gate_and_up",
        compiler_params=pltpu.CompilerParams(vmem_limit_bytes=16 * 2**20),
        cost_estimate=pl.CostEstimate(
            flops=2 * blocks * units * block * rows, bytes_accessed=2 * blocks * units * block, transcendentals=0
        ),
    )(order, *wide, middle)


def per_device(
    tokens,
    lengths,
    memory,
    norm_attn,
    w_query,
    w_key,
    w_value,
    w_gate,
    head_gain,
    w_out,
    norm_mlp,
    w_gate_mlp,
    w_up,
    w_down,
):
    f32, bf16 = jnp.float32, jnp.bfloat16
    n_kv, n_tp = lax.axis_size("kv"), lax.axis_size("tp")
    rows = tokens.shape[0]
    own = memory.shape[0]
    heads_local = memory.shape[1]
    head_size = memory.shape[2]
    width = w_query.shape[1]
    block = w_query.shape[0]
    ff = w_up.shape[1]

    tok = tokens.T
    gathered = lax.all_gather(tok, "tp", axis=0, tiled=True)
    wide_tok = gathered.astype(f32)
    squares = jnp.sum(wide_tok * wide_tok, axis=0)
    gain = norm_attn.astype(f32)[:, None]
    parts = jnp.concatenate(
        [
            lax.dot_general(
                gathered,
                (w.astype(f32) * gain).astype(bf16),
                (((0,), (0,)), ((), ())),
                preferred_element_type=f32,
            )
            for w in (w_query, w_key, w_value, w_gate)
        ],
        axis=1,
    ).astype(bf16)
    terms = jnp.stack([t.reshape(n_kv, own) for t in in_three(squares)], axis=1)
    terms = jnp.pad(terms, ((0, 0), (0, 1), (0, parts.shape[1] - own)))
    sent = jnp.concatenate([parts.reshape(n_kv, own, -1), terms], axis=1)
    got = lax.all_to_all(sent, "kv", 0, 0, tiled=True)
    summed = jnp.sum(got.astype(f32), axis=0)
    own_squares = summed[own, :own] + summed[own + 1, :own] + summed[own + 2, :own]
    projected = summed[:own] * lax.rsqrt(own_squares / D + epsilon)[:, None]

    half = head_size // 2
    inverse = 10000.0 ** (-jnp.arange(half, dtype=f32) / half)
    angles = lengths.astype(f32)[:, None] * inverse[None, :]
    cosine, sine = jnp.cos(angles)[:, None, :], jnp.sin(angles)[:, None, :]
    heads = [
        projected[:, i * width : (i + 1) * width].reshape(own, heads_local, head_size)
        for i in range(3)
    ]
    decay_rate = head_decay(lax.axis_index("tp") * heads_local + jnp.arange(heads_local))
    new_memory, mixed = retain(
        memory,
        rotate(heads[0], cosine, sine),
        rotate(heads[1], cosine, sine),
        heads[2],
        projected[:, 3 * width :],
        head_gain,
        decay_rate,
    )

    four = 4
    fours = n_kv // four
    near = [[a * four + i for i in range(four)] for a in range(fours)]
    far = [[a * four + i for a in range(fours)] for i in range(four)]
    share = ff // n_kv
    place = lax.rem(lax.axis_index("kv"), four)
    order = lax.bitwise_xor(place, jnp.arange(four))
    gain = norm_mlp.astype(f32)[:, None]
    wide = jnp.stack([(w.astype(f32) * gain).astype(bf16).T for w in (w_gate_mlp, w_up)])
    wide = wide.reshape(2, fours, four, share, block).transpose(2, 0, 1, 3, 4)
    wide = wide.reshape(four, 2 * fours * share, block)
    wide = [lax.dynamic_index_in_dim(wide, order[j], 0, keepdims=False) for j in range(four)]
    wide = [wide[0]] + [
        lax.ppermute(wide[j], "kv", [(k, k ^ j) for k in range(n_kv)]) for j in range(1, four)
    ]

    mixed_all = from_everyone(mixed, "kv").reshape(rows, width)
    attn_part = lax.dot_general(
        w_out, mixed_all, (((0,), (1,)), ((), ())), preferred_element_type=f32
    ).astype(bf16)
    attn = lax.all_to_all(attn_part.reshape(n_tp, -1, rows), "tp", 0, 0, tiled=True)
    middle = (tok.astype(f32) + jnp.sum(attn.astype(f32), axis=0)).astype(bf16)

    copies = jnp.broadcast_to(middle, (four, *middle.shape))
    mid_near = lax.all_to_all(copies, "kv", 0, 0, axis_index_groups=near, tiled=True)
    mid_all = lax.all_gather(mid_near, "tp", axis=1, tiled=True)
    both = gate_and_up(order, wide, mid_all, fours)
    both = lax.all_to_all(both, "kv", 0, 0, axis_index_groups=far, tiled=True)
    both = jnp.sum(both.astype(f32), axis=0)
    totals = both[share, :rows] + both[share, rows:] + both[share + 1, :rows]
    inv_mlp = lax.rsqrt(totals / D + epsilon)[None]
    hidden = jax.nn.silu(inv_mlp * both[:share, :rows]) * (inv_mlp * both[:share, rows:])
    hidden = lax.all_gather(hidden.astype(bf16), "kv", axis=0, tiled=True)
    down = lax.dot_general(
        w_down, hidden, (((0,), (0,)), ((), ())), preferred_element_type=f32
    ).astype(bf16)
    down = lax.all_to_all(down.reshape(n_tp, -1, rows), "tp", 0, 0, tiled=True)
    result = (middle.astype(f32) + jnp.sum(down.astype(f32), axis=0)).astype(bf16)
    return (result.T, new_memory)


def solution(mesh):
    in_specs = (
        P("grp", ("kv", "tp")),
        P(("grp", "kv")),
        P(("grp", "kv"), "tp", None, None),
        P("kv"),
        P("kv", "tp"),
        P("kv", "tp"),
        P("kv", "tp"),
        P("kv", "tp"),
        P("tp"),
        P("tp", "kv"),
        P("kv"),
        P("kv", "tp"),
        P("kv", "tp"),
        P("tp", "kv"),
    )
    out_specs = (P("grp", ("kv", "tp")), P(("grp", "kv"), "tp", None, None))
    return jax.shard_map(
        per_device, mesh=mesh, in_specs=in_specs, out_specs=out_specs, check_vma=False
    )
```

```python
import jax
import jax.numpy as jnp
from jax import lax
from jax.experimental import pallas as pl
from jax.experimental.pallas import tpu as pltpu
from jax.sharding import PartitionSpec as P


D = 4096
HEADS = 16


epsilon = 1e-06


def from_everyone(array, axis):
    copies = jnp.broadcast_to(array, (lax.axis_size(axis), *array.shape))
    return lax.all_to_all(copies, axis, split_axis=0, concat_axis=0, tiled=True)


def in_three(values):
    high = values.astype(jnp.bfloat16)
    rest = values - high.astype(jnp.float32)
    mid = rest.astype(jnp.bfloat16)
    low = (rest - mid.astype(jnp.float32)).astype(jnp.bfloat16)
    return high, mid, low


def rotate(values, cosine, sine):
    half_width = values.shape[-1] // 2
    first = values[..., :half_width]
    second = values[..., half_width:]
    return jnp.concatenate(
        [first * cosine - second * sine, second * cosine + first * sine], axis=-1
    )


def head_decay(head_index):
    exponent = -5.0 - head_index.astype(jnp.float32) * (7.0 / max(HEADS - 1, 1))
    return 1.0 - jnp.exp2(exponent)


def retain(memory, queries, key_rows, value_rows, gate_rows, head_gain, decay_rate):
    new_memory = (
        decay_rate[None, :, None, None] * memory
        + key_rows[:, :, :, None] * value_rows[:, :, None, :]
    )
    readout = jnp.einsum(
        "bhd,bhde->bhe",
        queries * queries.shape[-1] ** (-0.5),
        new_memory,
        precision=lax.Precision.HIGHEST,
    )
    centred = readout - jnp.mean(readout, axis=-1, keepdims=True)
    normed = centred * lax.rsqrt(jnp.mean(centred * centred, axis=-1, keepdims=True) + epsilon)
    normed = normed.reshape(readout.shape[0], -1) * head_gain.astype(jnp.float32)
    return (new_memory, (normed * jax.nn.silu(gate_rows)).astype(jnp.bfloat16))


def gate_and_up(order, wide, middle, parts):
    blocks = len(wide)
    units, block = wide[0].shape
    rows = middle.shape[2]
    share = units // (2 * parts)
    tail = 8

    def kernel(order_ref, *refs):
        wide_refs, middle_ref, out_ref = refs[:blocks], refs[blocks], refs[blocks + 1]
        total, squares = None, None
        for m in range(blocks):
            held = middle_ref[order_ref[m]]
            value = held.astype(jnp.float32)
            square = jnp.sum(value * value, axis=0, keepdims=True)
            product = jnp.dot(wide_refs[m][...], held, preferred_element_type=jnp.float32)
            total = product if total is None else total + product
            squares = square if squares is None else squares + square
        total = total.astype(jnp.bfloat16)
        high, mid, low = in_three(squares)
        ones = [high, mid, low, jnp.zeros_like(low)]
        under = jnp.concatenate(
            [
                jnp.concatenate([ones[2 * r].astype(jnp.float32), ones[2 * r + 1].astype(jnp.float32)], axis=1)
                for r in range(2)
            ]
            + [jnp.zeros((tail - 2, 2 * rows), jnp.float32)],
            axis=0,
        ).astype(jnp.bfloat16)
        for a in range(parts):
            for half in range(2):
                start = (half * parts + a) * share
                out_ref[a, :share, half * rows : (half + 1) * rows] = total[start : start + share]
            out_ref[a, share:, :] = under

    vmem = pl.BlockSpec(memory_space=pltpu.VMEM)
    return pl.pallas_call(
        kernel,
        out_shape=jax.ShapeDtypeStruct((parts, share + tail, 2 * rows), jnp.bfloat16),
        in_specs=[pl.BlockSpec(memory_space=pltpu.SMEM)] + [vmem] * (blocks + 1),
        out_specs=vmem,
        name="gate_and_up",
        compiler_params=pltpu.CompilerParams(vmem_limit_bytes=16 * 2**20),
        cost_estimate=pl.CostEstimate(
            flops=2 * blocks * units * block * rows, bytes_accessed=2 * blocks * units * block, transcendentals=0
        ),
    )(order, *wide, middle)


def per_device(
    tokens,
    lengths,
    memory,
    norm_attn,
    w_query,
    w_key,
    w_value,
    w_gate,
    head_gain,
    w_out,
    norm_mlp,
    w_gate_mlp,
    w_up,
    w_down,
):
    f32, bf16 = jnp.float32, jnp.bfloat16
    n_kv, n_tp = lax.axis_size("kv"), lax.axis_size("tp")
    rows = tokens.shape[0]
    own = memory.shape[0]
    heads_local = memory.shape[1]
    head_size = memory.shape[2]
    width = w_query.shape[1]
    block = w_query.shape[0]
    ff = w_up.shape[1]

    tok = tokens.T
    gathered = lax.all_gather(tok, "tp", axis=0, tiled=True)
    wide_tok = gathered.astype(f32)
    squares = jnp.sum(wide_tok * wide_tok, axis=0)
    gain = norm_attn.astype(f32)[:, None]
    parts = jnp.concatenate(
        [
            lax.dot_general(
                gathered,
                (w.astype(f32) * gain).astype(bf16),
                (((0,), (0,)), ((), ())),
                preferred_element_type=f32,
            )
            for w in (w_query, w_key, w_value, w_gate)
        ],
        axis=1,
    ).astype(bf16)
    terms = jnp.stack([t.reshape(n_kv, own) for t in in_three(squares)], axis=1)
    terms = jnp.pad(terms, ((0, 0), (0, 1), (0, parts.shape[1] - own)))
    sent = jnp.concatenate([parts.reshape(n_kv, own, -1), terms], axis=1)
    got = lax.all_to_all(sent, "kv", 0, 0, tiled=True)
    summed = jnp.sum(got.astype(f32), axis=0)
    own_squares = summed[own, :own] + summed[own + 1, :own] + summed[own + 2, :own]
    projected = summed[:own] * lax.rsqrt(own_squares / D + epsilon)[:, None]

    half = head_size // 2
    inverse = 10000.0 ** (-jnp.arange(half, dtype=f32) / half)
    angles = lengths.astype(f32)[:, None] * inverse[None, :]
    cosine, sine = jnp.cos(angles)[:, None, :], jnp.sin(angles)[:, None, :]
    heads = [
        projected[:, i * width : (i + 1) * width].reshape(own, heads_local, head_size)
        for i in range(3)
    ]
    decay_rate = head_decay(lax.axis_index("tp") * heads_local + jnp.arange(heads_local))
    new_memory, mixed = retain(
        memory,
        rotate(heads[0], cosine, sine),
        rotate(heads[1], cosine, sine),
        heads[2],
        projected[:, 3 * width :],
        head_gain,
        decay_rate,
    )

    four = 4
    fours = n_kv // four
    near = [[a * four + i for i in range(four)] for a in range(fours)]
    far = [[a * four + i for a in range(fours)] for i in range(four)]
    share = ff // n_kv
    place = lax.div(lax.axis_index("kv"), four)
    order = lax.bitwise_xor(place, jnp.arange(fours))
    gain = norm_mlp.astype(f32)[:, None]
    wide = jnp.stack([(w.astype(f32) * gain).astype(bf16).T for w in (w_gate_mlp, w_up)])
    wide = wide.reshape(2, fours, four * share, block).transpose(1, 0, 2, 3)
    wide = wide.reshape(fours, 2 * four * share, block)
    wide = [lax.dynamic_index_in_dim(wide, order[j], 0, keepdims=False) for j in range(fours)]
    wide = [wide[0]] + [
        lax.ppermute(wide[j], "kv", [(k, k ^ (j * four)) for k in range(n_kv)])
        for j in range(1, fours)
    ]

    mixed_all = from_everyone(mixed, "kv").reshape(rows, width)
    attn_part = lax.dot_general(
        w_out, mixed_all, (((0,), (1,)), ((), ())), preferred_element_type=f32
    ).astype(bf16)
    attn = lax.all_to_all(attn_part.reshape(n_tp, -1, rows), "tp", 0, 0, tiled=True)
    middle = (tok.astype(f32) + jnp.sum(attn.astype(f32), axis=0)).astype(bf16)

    copies = jnp.broadcast_to(middle, (fours, *middle.shape))
    mid_far = lax.all_to_all(copies, "kv", 0, 0, axis_index_groups=far, tiled=True)
    mid_all = lax.all_gather(mid_far, "tp", axis=1, tiled=True)
    both = gate_and_up(order, wide, mid_all, four)
    both = lax.all_to_all(both, "kv", 0, 0, axis_index_groups=near, tiled=True)
    both = jnp.sum(both.astype(f32), axis=0)
    totals = both[share, :rows] + both[share, rows:] + both[share + 1, :rows]
    inv_mlp = lax.rsqrt(totals / D + epsilon)[None]
    hidden = jax.nn.silu(inv_mlp * both[:share, :rows]) * (inv_mlp * both[:share, rows:])
    hidden = lax.all_gather(hidden.astype(bf16), "kv", axis=0, tiled=True)
    down = lax.dot_general(
        w_down, hidden, (((0,), (0,)), ((), ())), preferred_element_type=f32
    ).astype(bf16)
    down = lax.all_to_all(down.reshape(n_tp, -1, rows), "tp", 0, 0, tiled=True)
    result = (middle.astype(f32) + jnp.sum(down.astype(f32), axis=0)).astype(bf16)
    return (result.T, new_memory)


def solution(mesh):
    in_specs = (
        P("grp", ("kv", "tp")),
        P(("grp", "kv")),
        P(("grp", "kv"), "tp", None, None),
        P("kv"),
        P("kv", "tp"),
        P("kv", "tp"),
        P("kv", "tp"),
        P("kv", "tp"),
        P("tp"),
        P("tp", "kv"),
        P("kv"),
        P("kv", "tp"),
        P("kv", "tp"),
        P("tp", "kv"),
    )
    out_specs = (P("grp", ("kv", "tp")), P(("grp", "kv"), "tp", None, None))
    return jax.shard_map(
        per_device, mesh=mesh, in_specs=in_specs, out_specs=out_specs, check_vma=False
    )
```

```python
import jax
import jax.numpy as jnp
from jax import lax
from jax.experimental import pallas as pl
from jax.experimental.pallas import tpu as pltpu
from jax.sharding import PartitionSpec as P


D = 4096
HEADS = 16


epsilon = 1e-06


def in_three(values):
    high = values.astype(jnp.bfloat16)
    rest = values - high.astype(jnp.float32)
    mid = rest.astype(jnp.bfloat16)
    low = (rest - mid.astype(jnp.float32)).astype(jnp.bfloat16)
    return high, mid, low


def head_decay(head_index):
    exponent = -5.0 - head_index.astype(jnp.float32) * (7.0 / max(HEADS - 1, 1))
    return 1.0 - jnp.exp2(exponent)


VMEM = pl.BlockSpec(memory_space=pltpu.VMEM)
SMEM = pl.BlockSpec(memory_space=pltpu.SMEM)
LIMIT = pltpu.CompilerParams(vmem_limit_bytes=16 * 2**20)


def project(gathered, norm, weights, pieces):
    block, rows = gathered.shape
    width = weights[0].shape[1]
    count = len(weights)
    own = rows // pieces
    height = -(-(own + 3) // 8) * 8

    def kernel(tokens_ref, norm_ref, *refs):
        out_ref, held_ref, arrived = refs[count:]
        copies = [
            pltpu.make_async_copy(refs[c], held_ref.at[c], arrived.at[c]) for c in range(count)
        ]
        for copy in copies:
            copy.start()
        value = tokens_ref[...].astype(jnp.float32)
        squares = jnp.sum(value * value, axis=0, keepdims=True)
        gain = jnp.broadcast_to(norm_ref[...].astype(jnp.float32), (128, block)).T[:, :1]
        scaled = (value * gain).astype(jnp.bfloat16)
        under = [term.astype(jnp.float32) for term in in_three(squares)]
        under = jnp.concatenate(under + [jnp.zeros((height - own - 3, rows), jnp.float32)], axis=0)
        under = jnp.concatenate(
            [under, jnp.zeros((height - own, count * width - rows), jnp.float32)], axis=1
        )
        for c in range(count):
            copies[c].wait()
            product = lax.dot_general(
                scaled, held_ref[c], (((0,), (0,)), ((), ())), preferred_element_type=jnp.float32
            )
            span = slice(c * width, (c + 1) * width)
            for p in range(pieces):
                piece = jnp.concatenate([product[p * own : (p + 1) * own], under[:, span]], axis=0)
                out_ref[p, :, span] = piece.astype(jnp.bfloat16)

    return pl.pallas_call(
        kernel,
        out_shape=jax.ShapeDtypeStruct((pieces, height, count * width), jnp.bfloat16),
        in_specs=[VMEM] * 2 + [pl.BlockSpec(memory_space=pl.ANY)] * count,
        out_specs=VMEM,
        scratch_shapes=[
            pltpu.VMEM((count, block, width), jnp.bfloat16),
            pltpu.SemaphoreType.DMA((count,)),
        ],
        name="project",
        compiler_params=LIMIT,
        cost_estimate=pl.CostEstimate(
            flops=2 * count * block * width * rows, bytes_accessed=2 * gathered.size, transcendentals=0
        ),
    )(gathered, norm, *weights)


def attend(scalars, start, parts, cosine, sine, memory, head_gain, rows):
    pieces, _, _ = parts.shape
    own, size, _ = memory.shape

    def kernel(scalars_ref, start_ref, parts_ref, cos_ref, sin_ref, memory_ref, gain_ref, *refs):
        mixed_ref, keys_ref, values_ref, read_ref = refs
        summed = parts_ref[0].astype(jnp.float32)
        for p in range(1, pieces):
            summed = summed + parts_ref[p].astype(jnp.float32)
        total = summed[own : own + 1, :rows] + summed[own + 1 : own + 2, :rows]
        total = total + summed[own + 2 : own + 3, :rows]
        lane = lax.broadcasted_iota(jnp.int32, (own, rows), 1)
        line = lax.broadcasted_iota(jnp.int32, (own, rows), 0) + start_ref[0]
        total = jnp.sum(jnp.where(lane == line, total, 0.0), axis=1, keepdims=True)
        scale = lax.rsqrt(total / D + epsilon)
        query, key, value, gate = (
            summed[:own, i * size : (i + 1) * size] * scale for i in range(4)
        )
        query, key = (
            x * cos_ref[...] + pltpu.roll(x, size // 2, 1) * sin_ref[...] for x in (query, key)
        )
        query = query * size ** (-0.5)
        columns = jnp.concatenate([query, jnp.zeros((size - own, size), jnp.float32)], axis=0).T
        for b in range(own):
            read_ref[b : b + 1] = jnp.sum(columns[:, b : b + 1] * memory_ref[b], axis=0, keepdims=True)
        decay = scalars_ref[0]
        readout = decay * read_ref[...] + jnp.sum(query * key, axis=1, keepdims=True) * value
        centred = readout - jnp.mean(readout, axis=1, keepdims=True)
        normed = centred * lax.rsqrt(jnp.mean(centred * centred, axis=1, keepdims=True) + epsilon)
        normed = normed * gain_ref[...].astype(jnp.float32)
        mixed = (normed * (gate / (1.0 + jnp.exp(-gate)))).astype(jnp.bfloat16)
        for p in range(pieces):
            mixed_ref[p] = mixed
        keys_ref[...] = key
        values_ref[...] = value

    rows_type = jax.ShapeDtypeStruct((own, size), jnp.float32)
    return pl.pallas_call(
        kernel,
        out_shape=(jax.ShapeDtypeStruct((pieces, own, size), jnp.bfloat16), rows_type, rows_type),
        in_specs=[SMEM, SMEM] + [VMEM] * 5,
        out_specs=(VMEM,) * 3,
        scratch_shapes=[pltpu.VMEM((own, size), jnp.float32)],
        name="attend",
        compiler_params=LIMIT,
        cost_estimate=pl.CostEstimate(
            flops=2 * memory.size, bytes_accessed=4 * memory.size, transcendentals=2 * own * size
        ),
    )(scalars, start, parts, cosine, sine, memory, head_gain)


def gate_and_up(order, wide, middle, parts):
    blocks = len(wide)
    units, block = wide[0].shape
    rows = middle.shape[2]
    share = units // (2 * parts)
    tail = 8

    def kernel(order_ref, *refs):
        wide_refs, middle_ref, out_ref = refs[:blocks], refs[blocks], refs[blocks + 1]
        total, squares = None, None
        for m in range(blocks):
            held = middle_ref[order_ref[m]]
            value = held.astype(jnp.float32)
            square = jnp.sum(value * value, axis=0, keepdims=True)
            product = jnp.dot(wide_refs[m][...], held, preferred_element_type=jnp.float32)
            total = product if total is None else total + product
            squares = square if squares is None else squares + square
        total = total.astype(jnp.bfloat16)
        high, mid, low = in_three(squares)
        ones = [high, mid, low, jnp.zeros_like(low)]
        under = jnp.concatenate(
            [
                jnp.concatenate([ones[2 * r].astype(jnp.float32), ones[2 * r + 1].astype(jnp.float32)], axis=1)
                for r in range(2)
            ]
            + [jnp.zeros((tail - 2, 2 * rows), jnp.float32)],
            axis=0,
        ).astype(jnp.bfloat16)
        for a in range(parts):
            for half in range(2):
                start = (half * parts + a) * share
                out_ref[a, :share, half * rows : (half + 1) * rows] = total[start : start + share]
            out_ref[a, share:, :] = under

    return pl.pallas_call(
        kernel,
        out_shape=jax.ShapeDtypeStruct((parts, share + tail, 2 * rows), jnp.bfloat16),
        in_specs=[SMEM] + [VMEM] * (blocks + 1),
        out_specs=VMEM,
        name="gate_and_up",
        compiler_params=LIMIT,
        cost_estimate=pl.CostEstimate(
            flops=2 * blocks * units * block * rows, bytes_accessed=2 * blocks * units * block, transcendentals=0
        ),
    )(order, *wide, middle)


def per_device(
    tokens,
    lengths,
    memory,
    norm_attn,
    w_query,
    w_key,
    w_value,
    w_gate,
    head_gain,
    w_out,
    norm_mlp,
    w_gate_mlp,
    w_up,
    w_down,
):
    f32, bf16 = jnp.float32, jnp.bfloat16
    n_kv, n_tp = lax.axis_size("kv"), lax.axis_size("tp")
    rows = tokens.shape[0]
    own = memory.shape[0]
    heads_local = memory.shape[1]
    head_size = memory.shape[2]
    width = w_query.shape[1]
    block = w_query.shape[0]
    ff = w_up.shape[1]

    tok = tokens.T
    gathered = lax.all_gather(tok, "tp", axis=0, tiled=True)
    sent = project(gathered, norm_attn[None], (w_query, w_key, w_value, w_gate), n_kv)
    got = lax.all_to_all(sent, "kv", 0, 0, tiled=True)

    half = head_size // 2
    inverse = 10000.0 ** (-jnp.arange(half, dtype=f32) / half)
    angles = lengths.astype(f32)[:, None] * inverse[None, :]
    cosine, sine = jnp.cos(angles), jnp.sin(angles)
    cosine = jnp.concatenate([cosine, cosine], axis=1)
    sine = jnp.concatenate([-sine, sine], axis=1)
    decay_rate = head_decay(lax.axis_index("tp") * heads_local + jnp.arange(heads_local))
    start = (lax.axis_index("kv") * own)[None]
    mixed, keys, values = attend(
        decay_rate, start, got, cosine, sine, memory[:, 0], head_gain[None], rows
    )
    new_memory = (
        decay_rate[None, :, None, None] * memory + (keys[:, :, None] * values[:, None, :])[:, None]
    )

    four = 4
    fours = n_kv // four
    near = [[a * four + i for i in range(four)] for a in range(fours)]
    far = [[a * four + i for a in range(fours)] for i in range(four)]
    share = ff // n_kv
    place = lax.rem(lax.axis_index("kv"), four)
    order = lax.bitwise_xor(place, jnp.arange(four))
    gain = norm_mlp.astype(f32)[:, None]
    wide = jnp.stack([(w.astype(f32) * gain).astype(bf16).T for w in (w_gate_mlp, w_up)])
    wide = wide.reshape(2, fours, four, share, block).transpose(2, 0, 1, 3, 4)
    wide = wide.reshape(four, 2 * fours * share, block)
    wide = [lax.dynamic_index_in_dim(wide, order[j], 0, keepdims=False) for j in range(four)]
    wide = [wide[0]] + [
        lax.ppermute(wide[j], "kv", [(k, k ^ j) for k in range(n_kv)]) for j in range(1, four)
    ]

    mixed_all = lax.all_to_all(mixed, "kv", 0, 0, tiled=True).reshape(rows, width)
    attn_part = lax.dot_general(
        w_out, mixed_all, (((0,), (1,)), ((), ())), preferred_element_type=f32
    ).astype(bf16)
    attn = lax.all_to_all(attn_part.reshape(n_tp, -1, rows), "tp", 0, 0, tiled=True)
    middle = (tok.astype(f32) + jnp.sum(attn.astype(f32), axis=0)).astype(bf16)

    copies = jnp.broadcast_to(middle, (four, *middle.shape))
    mid_near = lax.all_to_all(copies, "kv", 0, 0, axis_index_groups=near, tiled=True)
    mid_all = lax.all_gather(mid_near, "tp", axis=1, tiled=True)
    both = gate_and_up(order, wide, mid_all, fours)
    both = lax.all_to_all(both, "kv", 0, 0, axis_index_groups=far, tiled=True)
    both = jnp.sum(both.astype(f32), axis=0)
    totals = both[share, :rows] + both[share, rows:] + both[share + 1, :rows]
    inv_mlp = lax.rsqrt(totals / D + epsilon)[None]
    hidden = jax.nn.silu(inv_mlp * both[:share, :rows]) * (inv_mlp * both[:share, rows:])
    hidden = lax.all_gather(hidden.astype(bf16), "kv", axis=0, tiled=True)
    down = lax.dot_general(
        w_down, hidden, (((0,), (0,)), ((), ())), preferred_element_type=f32
    ).astype(bf16)
    down = lax.all_to_all(down.reshape(n_tp, -1, rows), "tp", 0, 0, tiled=True)
    result = (middle.astype(f32) + jnp.sum(down.astype(f32), axis=0)).astype(bf16)
    return (result.T, new_memory)


def solution(mesh):
    in_specs = (
        P("grp", ("kv", "tp")),
        P(("grp", "kv")),
        P(("grp", "kv"), "tp", None, None),
        P("kv"),
        P("kv", "tp"),
        P("kv", "tp"),
        P("kv", "tp"),
        P("kv", "tp"),
        P("tp"),
        P("tp", "kv"),
        P("kv"),
        P("kv", "tp"),
        P("kv", "tp"),
        P("tp", "kv"),
    )
    out_specs = (P("grp", ("kv", "tp")), P(("grp", "kv"), "tp", None, None))
    return jax.shard_map(
        per_device, mesh=mesh, in_specs=in_specs, out_specs=out_specs, check_vma=False
    )
```

```python
import jax
import jax.numpy as jnp
from jax import lax
from jax.experimental import pallas as pl
from jax.experimental.pallas import tpu as pltpu
from jax.sharding import PartitionSpec as P


D = 4096
HEADS = 16


epsilon = 1e-06


def in_three(values):
    high = values.astype(jnp.bfloat16)
    rest = values - high.astype(jnp.float32)
    mid = rest.astype(jnp.bfloat16)
    low = (rest - mid.astype(jnp.float32)).astype(jnp.bfloat16)
    return high, mid, low


def head_decay(head_index):
    exponent = -5.0 - head_index.astype(jnp.float32) * (7.0 / max(HEADS - 1, 1))
    return 1.0 - jnp.exp2(exponent)


VMEM = pl.BlockSpec(memory_space=pltpu.VMEM)
SMEM = pl.BlockSpec(memory_space=pltpu.SMEM)
LIMIT = pltpu.CompilerParams(vmem_limit_bytes=16 * 2**20)


def project(gathered, weights, pieces):
    block, rows = gathered.shape
    count, _, width = weights.shape
    own = rows // pieces
    lines = -(-rows // width)
    height = -(-(count * own + 2 * lines) // 8) * 8

    def kernel(tokens_ref, weights_ref, out_ref):
        held = tokens_ref[...]
        value = held.astype(jnp.float32)
        squares = jnp.sum(value * value, axis=0, keepdims=True)
        squares = jnp.concatenate(
            [squares, jnp.zeros((1, lines * width - rows), jnp.float32)], axis=1
        )
        terms = [term.astype(jnp.float32) for term in in_three(squares)[:2]]
        under = jnp.concatenate(
            [term[:, i * width : (i + 1) * width] for term in terms for i in range(lines)]
            + [jnp.zeros((height - count * own - 2 * lines, width), jnp.float32)],
            axis=0,
        )
        products = [
            lax.dot_general(
                held, weights_ref[c], (((0,), (0,)), ((), ())), preferred_element_type=jnp.float32
            )
            for c in range(count)
        ]
        for p in range(pieces):
            piece = [product[p * own : (p + 1) * own] for product in products]
            out_ref[p] = jnp.concatenate(piece + [under], axis=0).astype(jnp.bfloat16)

    return pl.pallas_call(
        kernel,
        out_shape=jax.ShapeDtypeStruct((pieces, height, width), jnp.bfloat16),
        in_specs=[VMEM] * 2,
        out_specs=VMEM,
        name="project",
        compiler_params=LIMIT,
        cost_estimate=pl.CostEstimate(
            flops=2 * count * block * width * rows, bytes_accessed=2 * gathered.size, transcendentals=0
        ),
    )(gathered, weights)


def attend(scalars, start, parts, cosine, sine, memory, head_gain, rows):
    pieces = parts.shape[0]
    own, size, _ = memory.shape
    lines = -(-rows // size)

    def kernel(scalars_ref, start_ref, parts_ref, cos_ref, sin_ref, memory_ref, gain_ref, *refs):
        mixed_ref, keys_ref, values_ref, read_ref = refs
        summed = parts_ref[0].astype(jnp.float32)
        for p in range(1, pieces):
            summed = summed + parts_ref[p].astype(jnp.float32)
        total = summed[4 * own : 4 * own + lines] + summed[4 * own + lines : 4 * own + 2 * lines]
        total = jnp.concatenate([total[i : i + 1] for i in range(lines)], axis=1)
        lane = lax.broadcasted_iota(jnp.int32, (own, lines * size), 1)
        line = lax.broadcasted_iota(jnp.int32, (own, lines * size), 0) + start_ref[0]
        total = jnp.sum(jnp.where(lane == line, total, 0.0), axis=1, keepdims=True)
        scale = lax.rsqrt(total / D + epsilon)
        query, key, value, gate = (
            summed[i * own : (i + 1) * own] * scale for i in range(4)
        )
        query, key = (
            x * cos_ref[...] + pltpu.roll(x, size // 2, 1) * sin_ref[...] for x in (query, key)
        )
        query = query * size ** (-0.5)
        columns = jnp.concatenate([query, jnp.zeros((size - own, size), jnp.float32)], axis=0).T
        for b in range(own):
            read_ref[b : b + 1] = jnp.sum(columns[:, b : b + 1] * memory_ref[b], axis=0, keepdims=True)
        decay = scalars_ref[0]
        readout = decay * read_ref[...] + jnp.sum(query * key, axis=1, keepdims=True) * value
        centred = readout - jnp.mean(readout, axis=1, keepdims=True)
        normed = centred * lax.rsqrt(jnp.mean(centred * centred, axis=1, keepdims=True) + epsilon)
        normed = normed * gain_ref[...].astype(jnp.float32)
        mixed = (normed * (gate / (1.0 + jnp.exp(-gate)))).astype(jnp.bfloat16)
        for p in range(pieces):
            mixed_ref[p] = mixed
        keys_ref[...] = key
        values_ref[...] = value

    rows_type = jax.ShapeDtypeStruct((own, size), jnp.float32)
    return pl.pallas_call(
        kernel,
        out_shape=(jax.ShapeDtypeStruct((pieces, own, size), jnp.bfloat16), rows_type, rows_type),
        in_specs=[SMEM, SMEM] + [VMEM] * 5,
        out_specs=(VMEM,) * 3,
        scratch_shapes=[pltpu.VMEM((own, size), jnp.float32)],
        name="attend",
        compiler_params=LIMIT,
        cost_estimate=pl.CostEstimate(
            flops=2 * memory.size, bytes_accessed=4 * memory.size, transcendentals=2 * own * size
        ),
    )(scalars, start, parts, cosine, sine, memory, head_gain)


def gate_and_up(order, wide, middle, parts):
    blocks = len(wide)
    units, block = wide[0].shape
    rows = middle.shape[2]
    share = units // (2 * parts)
    tail = 8

    def kernel(order_ref, *refs):
        wide_refs, middle_ref, out_ref = refs[:blocks], refs[blocks], refs[blocks + 1]
        total, squares = None, None
        for m in range(blocks):
            held = middle_ref[order_ref[m]]
            value = held.astype(jnp.float32)
            square = jnp.sum(value * value, axis=0, keepdims=True)
            product = jnp.dot(wide_refs[m][...], held, preferred_element_type=jnp.float32)
            total = product if total is None else total + product
            squares = square if squares is None else squares + square
        total = total.astype(jnp.bfloat16)
        high, mid, low = in_three(squares)
        ones = [high, mid, low, jnp.zeros_like(low)]
        under = jnp.concatenate(
            [
                jnp.concatenate([ones[2 * r].astype(jnp.float32), ones[2 * r + 1].astype(jnp.float32)], axis=1)
                for r in range(2)
            ]
            + [jnp.zeros((tail - 2, 2 * rows), jnp.float32)],
            axis=0,
        ).astype(jnp.bfloat16)
        for a in range(parts):
            for half in range(2):
                start = (half * parts + a) * share
                out_ref[a, :share, half * rows : (half + 1) * rows] = total[start : start + share]
            out_ref[a, share:, :] = under

    return pl.pallas_call(
        kernel,
        out_shape=jax.ShapeDtypeStruct((parts, share + tail, 2 * rows), jnp.bfloat16),
        in_specs=[SMEM] + [VMEM] * (blocks + 1),
        out_specs=VMEM,
        name="gate_and_up",
        compiler_params=LIMIT,
        cost_estimate=pl.CostEstimate(
            flops=2 * blocks * units * block * rows, bytes_accessed=2 * blocks * units * block, transcendentals=0
        ),
    )(order, *wide, middle)


def per_device(
    tokens,
    lengths,
    memory,
    norm_attn,
    w_query,
    w_key,
    w_value,
    w_gate,
    head_gain,
    w_out,
    norm_mlp,
    w_gate_mlp,
    w_up,
    w_down,
):
    f32, bf16 = jnp.float32, jnp.bfloat16
    n_kv, n_tp = lax.axis_size("kv"), lax.axis_size("tp")
    rows = tokens.shape[0]
    own = memory.shape[0]
    heads_local = memory.shape[1]
    head_size = memory.shape[2]
    width = w_query.shape[1]
    block = w_query.shape[0]
    ff = w_up.shape[1]

    tok = tokens.T
    gathered = jnp.broadcast_to(tok, (n_tp, *tok.shape))
    gathered = lax.all_to_all(gathered, "tp", 0, 0, tiled=True).reshape(block, rows)
    gain = norm_attn.astype(f32)[:, None]
    folded = jnp.stack(
        [(w.astype(f32) * gain).astype(bf16) for w in (w_query, w_key, w_value, w_gate)]
    )
    sent = project(gathered, folded, n_kv)
    got = lax.all_to_all(sent, "kv", 0, 0, tiled=True)

    half = head_size // 2
    inverse = 10000.0 ** (-jnp.arange(half, dtype=f32) / half)
    angles = lengths.astype(f32)[:, None] * inverse[None, :]
    cosine, sine = jnp.cos(angles), jnp.sin(angles)
    cosine = jnp.concatenate([cosine, cosine], axis=1)
    sine = jnp.concatenate([-sine, sine], axis=1)
    decay_rate = head_decay(lax.axis_index("tp") * heads_local + jnp.arange(heads_local))
    start = (lax.axis_index("kv") * own)[None]
    mixed, keys, values = attend(
        decay_rate, start, got, cosine, sine, memory[:, 0], head_gain[None], rows
    )
    new_memory = (
        decay_rate[None, :, None, None] * memory + (keys[:, :, None] * values[:, None, :])[:, None]
    )

    four = 4
    fours = n_kv // four
    near = [[a * four + i for i in range(four)] for a in range(fours)]
    far = [[a * four + i for a in range(fours)] for i in range(four)]
    share = ff // n_kv
    place = lax.rem(lax.axis_index("kv"), four)
    order = lax.bitwise_xor(place, jnp.arange(four))
    gain = norm_mlp.astype(f32)[:, None]
    wide = jnp.stack([(w.astype(f32) * gain).astype(bf16).T for w in (w_gate_mlp, w_up)])
    wide = wide.reshape(2, fours, four, share, block).transpose(2, 0, 1, 3, 4)
    wide = wide.reshape(four, 2 * fours * share, block)
    wide = [lax.dynamic_index_in_dim(wide, order[j], 0, keepdims=False) for j in range(four)]
    wide = [wide[0]] + [
        lax.ppermute(wide[j], "kv", [(k, k ^ j) for k in range(n_kv)]) for j in range(1, four)
    ]

    mixed_all = lax.all_to_all(mixed, "kv", 0, 0, tiled=True).reshape(rows, width)
    attn_part = lax.dot_general(
        w_out, mixed_all, (((0,), (1,)), ((), ())), preferred_element_type=f32
    ).astype(bf16)
    attn = lax.all_to_all(attn_part.reshape(n_tp, -1, rows), "tp", 0, 0, tiled=True)
    middle = (tok.astype(f32) + jnp.sum(attn.astype(f32), axis=0)).astype(bf16)

    copies = jnp.broadcast_to(middle, (four, *middle.shape))
    mid_near = lax.all_to_all(copies, "kv", 0, 0, axis_index_groups=near, tiled=True)
    mid_all = lax.all_gather(mid_near, "tp", axis=1, tiled=True)
    both = gate_and_up(order, wide, mid_all, fours)
    both = lax.all_to_all(both, "kv", 0, 0, axis_index_groups=far, tiled=True)
    both = jnp.sum(both.astype(f32), axis=0)
    totals = both[share, :rows] + both[share, rows:] + both[share + 1, :rows]
    inv_mlp = lax.rsqrt(totals / D + epsilon)[None]
    hidden = jax.nn.silu(inv_mlp * both[:share, :rows]) * (inv_mlp * both[:share, rows:])
    hidden = lax.all_gather(hidden.astype(bf16), "kv", axis=0, tiled=True)
    down = lax.dot_general(
        w_down, hidden, (((0,), (0,)), ((), ())), preferred_element_type=f32
    ).astype(bf16)
    down = lax.all_to_all(down.reshape(n_tp, -1, rows), "tp", 0, 0, tiled=True)
    result = (middle.astype(f32) + jnp.sum(down.astype(f32), axis=0)).astype(bf16)
    return (result.T, new_memory)


def solution(mesh):
    in_specs = (
        P("grp", ("kv", "tp")),
        P(("grp", "kv")),
        P(("grp", "kv"), "tp", None, None),
        P("kv"),
        P("kv", "tp"),
        P("kv", "tp"),
        P("kv", "tp"),
        P("kv", "tp"),
        P("tp"),
        P("tp", "kv"),
        P("kv"),
        P("kv", "tp"),
        P("kv", "tp"),
        P("tp", "kv"),
    )
    out_specs = (P("grp", ("kv", "tp")), P(("grp", "kv"), "tp", None, None))
    return jax.shard_map(
        per_device, mesh=mesh, in_specs=in_specs, out_specs=out_specs, check_vma=False
    )
```
